32 devices in a mesh: rep: 2 (over y), fs: 4 (over z), tp: 4 (over x, core).
Axes of the slice: x: 2, y: 2, z: 4, core: 2. Of those that a mesh axis runs over, the one named last changes fastest.
Arguments:
- tokens: bfloat16 [2048, 2048], P(('rep', 'fs')), may hold values from -6 to 6
- gate_weight: bfloat16 [2048, 2816], P('fs', 'tp'), may hold values from -0.125 to 0.125
- up_weight: bfloat16 [2048, 2816], P('fs', 'tp'), may hold values from -0.125 to 0.125
- down_weight: bfloat16 [2816, 2048], P('tp', 'fs'), may hold values from -0.109375 to 0.109375
- out_grad: bfloat16 [2048, 2048], P(('rep', 'fs')), may hold values from -6 to 6
Outputs:
- input_grad: bfloat16 [2048, 2048], P(('rep', 'fs'))
- down_grad: float32 [2816, 2048], P('tp', 'fs')
- row_norms: float32 [2816], P('tp')
The draws below stay inside these ranges and needn't reach their ends.
All inputs are finite; a program needn't handle non-finite values.
Results may differ from the reference program's by a relative error of at most 0.024.
Values may be sent and summed in bfloat16 or wider, within the bound.
No kernel may reach another device: no remote copies, remote signals or barrier semaphores. Data moves between devices by JAX's collectives and lax.ppermute only.
A program may use at most 64 MiB of HBM per device.

```python
import jax
import jax.numpy as jnp
from jax import lax

D = 2048
FF = 2816
TOKENS = 2048
N_TP = 4


def spiked(drawn, rng, source, target, parts, factor):
    def block_of(axis_at):
        return (jnp.arange(drawn.shape[axis_at]) // (drawn.shape[axis_at] // parts)).reshape((-1,) + (1,) * (drawn.ndim - 1 - axis_at))

    first = jax.random.permutation(rng, parts)[block_of(target)]
    second = (block_of(target) + parts // 2) % parts
    return jnp.where((block_of(source) == first) | (block_of(source) == second), factor * drawn, drawn)


def steps_of(own_key, dims, split, least, largest):
    def one(dim, blocks):
        steps = jax.random.uniform(jax.random.fold_in(jax.random.fold_in(own_key, 6), dim), (blocks,), jnp.float32, least / len(split), largest / len(split))
        return jnp.repeat(jnp.exp(steps), dims[dim] // blocks).reshape((-1,) + (1,) * (len(dims) - dim - 1))

    loudness = one(*split[0])
    for cut in split[1:]:
        loudness = loudness * one(*cut)
    return loudness


def noise(stream_key, extent, width, most, pieces=(), kind=jnp.bfloat16):
    entries = jax.random.normal(stream_key, extent, jnp.float32) * width
    if len(pieces) > 0:
        entries = steps_of(stream_key, extent, pieces, -0.22, 0.18) * entries
    return jnp.clip(entries, min=-most, max=most).astype(kind)


def noise_with(rng, dims, scale, bound, cuts, heavy, held_as=jnp.bfloat16):
    drawn = scale * jax.random.normal(rng, dims, jnp.float32)
    if cuts:
        drawn = drawn * steps_of(rng, dims, cuts, -0.22, 0.18)
    return jnp.clip(spiked(drawn, jax.random.fold_in(rng, 3), *heavy), -bound, bound).astype(held_as)


def setup_inputs(seed: int = 0) -> dict:
    key_of = jax.random.split(jax.random.key(seed), 6)
    tokens = noise(key_of[0], (TOKENS, D), 1.0, 6.0, ((0, 8),))
    gate_weight = noise(key_of[1], (D, FF), D ** -0.5, 0.125, ((0, 4), (1, 4)))
    up_weight = noise(key_of[2], (D, FF), D ** -0.5, 0.125, ((0, 4), (1, 4)))
    down_weight = noise(key_of[3], (FF, D), FF ** -0.5, 0.109375, ((0, 4), (1, 4)))
    out_grad = noise_with(key_of[4], (TOKENS, D), 1.0, 6.0, ((0, 8),), (0, 1, 8, 2.0))
    return {"tokens": tokens, "gate_weight": gate_weight, "up_weight": up_weight, "down_weight": down_weight, "out_grad": out_grad}


def reference(tokens, gate_weight, up_weight, down_weight, out_grad):
    gate_pre = jnp.dot(tokens, gate_weight, preferred_element_type=jnp.float32)
    up_pre = jnp.dot(tokens, up_weight, preferred_element_type=jnp.float32)
    sigma = jax.nn.sigmoid(gate_pre)
    activated = gate_pre * sigma
    hidden = (activated * up_pre).astype(jnp.bfloat16)
    hid_grad = lax.dot_general(out_grad, down_weight, (((1,), (1,)), ((), ())), preferred_element_type=jnp.float32)
    up_grad = (hid_grad * activated).astype(jnp.bfloat16)
    gate_grad = (hid_grad * up_pre * sigma * (1.0 + gate_pre * (1.0 - sigma))).astype(jnp.bfloat16)
    block = FF // N_TP

    def add_block(index, total):
        offset = (index * block).astype(jnp.int32)
        gate_part = lax.dynamic_slice_in_dim(gate_grad, offset, block, 1)
        up_part = lax.dynamic_slice_in_dim(up_grad, offset, block, 1)
        gate_rows = lax.dynamic_slice_in_dim(gate_weight, offset, block, 1)
        up_rows = lax.dynamic_slice_in_dim(up_weight, offset, block, 1)
        partial_value = lax.dot_general(gate_part, gate_rows, (((1,), (1,)), ((), ())), preferred_element_type=jnp.float32)
        partial_value = partial_value + lax.dot_general(up_part, up_rows, (((1,), (1,)), ((), ())), preferred_element_type=jnp.float32)
        return total + partial_value.astype(jnp.bfloat16).astype(jnp.float32)

    total = lax.fori_loop(0, N_TP, add_block, jnp.zeros(tokens.shape, jnp.float32))
    input_grad = total.astype(jnp.bfloat16)
    down_grad = lax.dot_general(hidden, out_grad, (((0,), (0,)), ((), ())), preferred_element_type=jnp.float32)
    row_norms = jnp.sum(down_grad * down_grad, axis=1)
    return input_grad, down_grad, row_norms
```

```python
import jax
import jax.numpy as jnp
from jax import lax
from jax.sharding import PartitionSpec as P


F32, BF16 = jnp.float32, jnp.bfloat16


def contract_last(left, right):
    return lax.dot_general(left, right, (((1,), (1,)), ((), ())), preferred_element_type=F32)


def contract_first(left, right):
    return lax.dot_general(left, right, (((0,), (0,)), ((), ())), preferred_element_type=F32)


def gathered(tokens, gate_weight, up_weight, down_weight, out_grad):
    down_full = lax.all_gather(down_weight, "fs", axis=1, tiled=True)
    gate_full = lax.all_gather(gate_weight, "fs", axis=0, tiled=True)
    up_full = lax.all_gather(up_weight, "fs", axis=0, tiled=True)
    gate_pre = jnp.dot(tokens, gate_full, preferred_element_type=F32)
    up_pre = jnp.dot(tokens, up_full, preferred_element_type=F32)
    hid_grad = contract_last(out_grad, down_full)
    hidden, gate_grad, up_grad = pointwise(gate_pre, up_pre, hid_grad)
    partial_value = contract_last(gate_grad, gate_full) + contract_last(up_grad, up_full)
    input_grad = lax.psum(partial_value.astype(BF16), "tp")
    columns = lax.all_to_all(out_grad, "fs", split_axis=1, concat_axis=0, tiled=True)
    shard = contract_first(lax.all_gather(hidden, "fs", axis=0, tiled=True), columns)
    shard = lax.psum(shard.astype(BF16), "rep").astype(F32)
    norms = lax.psum(jnp.sum(shard * shard, axis=1), "fs")
    return input_grad, shard, norms


def pointwise(gate_pre, up_pre, hid_grad):
    sigma = jax.nn.sigmoid(gate_pre)
    activated = gate_pre * sigma
    hidden = (activated * up_pre).astype(BF16)
    up_grad = (hid_grad * activated).astype(BF16)
    gate_grad = (hid_grad * up_pre * sigma * (1.0 + gate_pre * (1.0 - sigma))).astype(BF16)
    return hidden, gate_grad, up_grad


OUTER_PAIRS = ((0, 1), (1, 0), (2, 3), (3, 2))
INWARD = ((0, 1), (3, 2))
OUTWARD = ((1, 0), (2, 3))
MIDDLE = ((1, 2), (2, 1))
SWAP = ((0, 1), (1, 0))
OVER_X = ((0, 2), (2, 0), (1, 3), (3, 1))
OVER_CORE = ((0, 1), (1, 0), (2, 3), (3, 2))


def send(value, axis, pairs):
    return lax.ppermute(value, axis, pairs)


def paired(tokens, gate_weight, up_weight, down_weight, out_grad):
    y, z, t = lax.axis_index("rep"), lax.axis_index("fs"), lax.axis_index("tp")
    rows, width = tokens.shape
    units, depth = down_weight.shape
    half, quarter = units // 2, rows // 4
    part = half // 2
    x_of, core_of = t // 2, t % 2
    inner = jnp.logical_and(z > 0, z < 3)

    far_inner = jnp.where(z < 2, 2, 1)
    far_outer = jnp.where(z < 2, 3, 0)
    places = (z, z + 1 - 2 * (z % 2), far_inner, far_outer)

    def my_half(w):
        return lax.dynamic_slice_in_dim(w, y * half, half, 0)

    gate_h, up_h, down_h = my_half(gate_weight.T), my_half(up_weight.T), my_half(down_weight)
    gu = [jnp.concatenate([gate_h[c * part:(c + 1) * part], up_h[c * part:(c + 1) * part]], 0) for c in range(2)]

    both = jnp.stack([tokens, out_grad], 0)
    mine = lax.dynamic_slice_in_dim(both, t * quarter, quarter, 1)
    q0 = send(mine, "rep", SWAP)

    first = [send(w, "fs", OUTER_PAIRS) for w in gu]
    mid = [send(w, "fs", MIDDLE) for w in gu]
    q1 = send(q0, "tp", OVER_X)
    first.append(send(down_h, "fs", OUTER_PAIRS))
    mid.append(send(down_h, "fs", MIDDLE))
    q01 = jnp.concatenate([q0, q1], 1)
    q23 = send(q01, "tp", OVER_CORE)
    other = jnp.concatenate([q01, q23], 1)
    x_all = jnp.concatenate([tokens, other[0]], 0)
    g_all = jnp.concatenate([out_grad, other[1]], 0)

    mid2 = [send(v, "fs", MIDDLE) for v in first]
    out1 = [send(v, "fs", OUTWARD) for v in mid]
    out2 = [send(v, "fs", OUTWARD) for v in mid2]
    own = gu + [down_h]

    def pieces(i):
        return (own[i], first[i], jnp.where(inner, mid[i], out1[i]), jnp.where(inner, mid2[i], out2[i]))

    def columns(a):
        return [lax.dynamic_slice_in_dim(a, p * depth, depth, 1) for p in places]

    x_cols, g_cols = columns(x_all), columns(g_all)

    def project(cols, ws):
        return sum(contract_last(c, w) for c, w in zip(cols, ws))

    gu_pieces = [pieces(0), pieces(1)]
    pres = [project(x_cols, ws) for ws in gu_pieces]
    finals = []
    for c in range(2):
        gate_pre, up_pre = pres[c][:, :part], pres[c][:, part:]
        hidden = (gate_pre * jax.nn.sigmoid(gate_pre) * up_pre).astype(BF16)
        own_b, pair_b, in_b, out_b = [contract_first(hidden, g) for g in g_cols]
        far = jnp.concatenate([in_b, out_b], 0)
        got = send(far.astype(BF16), "fs", INWARD)
        got = send((far + got.astype(F32)).astype(BF16), "fs", MIDDLE).astype(F32)
        last = send((pair_b + got[part:]).astype(BF16), "fs", OUTER_PAIRS).astype(F32)
        finals.append((own_b + got[:part] + last).astype(BF16))
    final_own = jnp.concatenate(finals, 0)
    peers = jnp.concatenate([send(f, "rep", SWAP) for f in finals], 0)
    low = jnp.where(y == 0, final_own, peers)
    high = jnp.where(y == 0, peers, final_own)
    down_grad = jnp.concatenate([low, high], 0).astype(F32)
    f32_own = final_own.astype(F32)
    norm = jnp.sum(f32_own * f32_own, axis=1, keepdims=True).reshape(1, half)
    norm = norm + send(norm, "fs", OUTER_PAIRS)
    norm = norm + send(norm, "fs", ((0, 3), (3, 0), (1, 2), (2, 1)))
    norm_peer = send(norm, "rep", SWAP)
    norms = jnp.concatenate([jnp.where(y == 0, norm, norm_peer), jnp.where(y == 0, norm_peer, norm)], 1).reshape(units)

    down_pieces = pieces(2)
    hid = project(g_cols, down_pieces)
    grads = []
    for c in range(2):
        _, gate_grad, up_grad = pointwise(pres[c][:, :part], pres[c][:, part:], hid[:, c * part:(c + 1) * part])
        grads.append(jnp.concatenate([gate_grad, up_grad], 1))
    blocks = [
        sum(jnp.dot(grads[c], gu_pieces[c][p], preferred_element_type=F32) for c in range(2)) for p in range(4)
    ]
    total = jnp.zeros((2 * rows, width), BF16)
    for p in range(4):
        total = lax.dynamic_update_slice(total, blocks[p].astype(BF16), (0, places[p] * depth))
    ours = total[:rows].reshape(2, 2, quarter, width)
    theirs = total[rows:].reshape(2, 2, quarter, width)
    keep = jnp.stack([lax.dynamic_index_in_dim(ours, core_of, 1, False), theirs[0]], 0)
    give = jnp.stack([lax.dynamic_index_in_dim(ours, 1 - core_of, 1, False), theirs[1]], 0)
    got = send(give, "tp", OVER_CORE)
    halved = keep.astype(F32) + got.astype(F32)
    keep_x = jnp.stack([lax.dynamic_index_in_dim(halved[0], x_of, 0, False), halved[1][0]], 0)
    give_x = jnp.stack([lax.dynamic_index_in_dim(halved[0], 1 - x_of, 0, False), halved[1][1]], 0)
    got = send(give_x.astype(BF16), "tp", OVER_X)
    summed = keep_x + got.astype(F32)
    got = send(summed[1].astype(BF16), "rep", SWAP)
    done = (summed[0] + got.astype(F32)).astype(BF16)
    done_x = send(done, "tp", OVER_X)
    pair = jnp.stack([jnp.where(x_of == 0, done, done_x), jnp.where(x_of == 0, done_x, done)], 0)
    pair_c = send(pair, "tp", OVER_CORE)
    input_grad = jnp.stack([jnp.where(core_of == 0, pair, pair_c), jnp.where(core_of == 0, pair_c, pair)], 1)
    return input_grad.reshape(rows, width), down_grad, norms


def solution(mesh):
    sizes = dict(mesh.shape)
    plan = paired if (sizes["rep"], sizes["fs"], sizes["tp"]) == (2, 4, 4) else gathered
    return jax.shard_map(
        plan,
        mesh=mesh,
        in_specs=(
            P(("rep", "fs"), None),
            P("fs", "tp"),
            P("fs", "tp"),
            P("tp", "fs"),
            P(("rep", "fs"), None),
        ),
        out_specs=(P(("rep", "fs"), None), P("tp", "fs"), P("tp")),
        check_vma=False,
    )
```

```python
import jax
import jax.numpy as jnp
from jax import lax
from jax.experimental import pallas as pl
from jax.experimental.pallas import tpu as pltpu
from jax.sharding import PartitionSpec as P


F32, BF16 = jnp.float32, jnp.bfloat16


def contract_last(left, right):
    return lax.dot_general(left, right, (((1,), (1,)), ((), ())), preferred_element_type=F32)


def contract_first(left, right):
    return lax.dot_general(left, right, (((0,), (0,)), ((), ())), preferred_element_type=F32)


def gathered(tokens, gate_weight, up_weight, down_weight, out_grad):
    down_full = lax.all_gather(down_weight, "fs", axis=1, tiled=True)
    gate_full = lax.all_gather(gate_weight, "fs", axis=0, tiled=True)
    up_full = lax.all_gather(up_weight, "fs", axis=0, tiled=True)
    gate_pre = jnp.dot(tokens, gate_full, preferred_element_type=F32)
    up_pre = jnp.dot(tokens, up_full, preferred_element_type=F32)
    hid_grad = contract_last(out_grad, down_full)
    hidden, gate_grad, up_grad = pointwise(gate_pre, up_pre, hid_grad)
    partial_value = contract_last(gate_grad, gate_full) + contract_last(up_grad, up_full)
    input_grad = lax.psum(partial_value.astype(BF16), "tp")
    columns = lax.all_to_all(out_grad, "fs", split_axis=1, concat_axis=0, tiled=True)
    shard = contract_first(lax.all_gather(hidden, "fs", axis=0, tiled=True), columns)
    shard = lax.psum(shard.astype(BF16), "rep").astype(F32)
    norms = lax.psum(jnp.sum(shard * shard, axis=1), "fs")
    return input_grad, shard, norms


def pointwise(gate_pre, up_pre, hid_grad):
    sigma = jax.nn.sigmoid(gate_pre)
    activated = gate_pre * sigma
    hidden = (activated * up_pre).astype(BF16)
    up_grad = (hid_grad * activated).astype(BF16)
    gate_grad = (hid_grad * up_pre * sigma * (1.0 + gate_pre * (1.0 - sigma))).astype(BF16)
    return hidden, gate_grad, up_grad


OUTER_PAIRS = ((0, 1), (1, 0), (2, 3), (3, 2))
INWARD = ((0, 1), (3, 2))
OUTWARD = ((1, 0), (2, 3))
MIDDLE = ((1, 2), (2, 1))
ACROSS = ((0, 3), (3, 0), (1, 2), (2, 1))
SWAP = ((0, 1), (1, 0))
OVER_X = ((0, 2), (2, 0), (1, 3), (3, 1))
OVER_CORE = ((0, 1), (1, 0), (2, 3), (3, 2))


def paired(tokens, gate_weight, up_weight, down_weight, out_grad):
    return paired_body(tokens, gate_weight, up_weight, down_weight, out_grad)


def line_places():
    z = lax.axis_index("fs")
    return z, z + 1 - 2 * (z % 2), jnp.where(z < 2, 2, 1), jnp.where(z < 2, 3, 0)


def is_inner():
    z = lax.axis_index("fs")
    return jnp.logical_and(z > 0, z < 3)


def token_quarters():
    t = lax.axis_index("tp")
    x, c = t // 2, t % 2
    return t, 2 * (1 - x) + c, 2 * x + 1 - c, 3 - t


def call(kernel, outs, scratch=(), flops=0, limit=28):
    def run(*args):
        size = sum(v.size * v.dtype.itemsize for v in args)
        return pl.pallas_call(
            kernel,
            out_shape=outs,
            in_specs=[pl.BlockSpec(memory_space=pltpu.VMEM)] * len(args),
            out_specs=[pl.BlockSpec(memory_space=pltpu.VMEM)] * len(outs),
            scratch_shapes=list(scratch),
            compiler_params=pltpu.CompilerParams(vmem_limit_bytes=limit * 2**20),
            cost_estimate=pl.CostEstimate(flops=flops, bytes_accessed=size, transcendentals=0),
        )(*args)

    return run


def like(shape, dtype):
    return jax.ShapeDtypeStruct(shape, dtype)


def lay_kernel(tok, grad, *refs):
    others, (xs, gs) = refs[:4], refs[4:]
    depth, quarter = xs.shape[2], others[0].shape[1]
    quarters = token_quarters()
    for p, place in enumerate(line_places()):
        cols = pl.ds(pl.multiple_of(place * depth, depth), depth)
        for i in range(4):
            rows = pl.ds(pl.multiple_of(quarters[i] * quarter, quarter), quarter)
            here, there = pl.ds(i * quarter, quarter), pl.ds((4 + i) * quarter, quarter)
            xs[p, here, :] = tok[rows, cols]
            gs[p, here, :] = grad[rows, cols]
            xs[p, there, :] = others[i][0, :, cols]
            gs[p, there, :] = others[i][1, :, cols]


def either(inner, a, b):
    return jnp.where(inner, a[...], b[...])


def dot(a, b):
    return jnp.dot(a, b, preferred_element_type=F32)


def project(ws, cols):
    return sum(contract_last(w, cols[p]) for p, w in enumerate(ws))


def front_kernel(xs, gs, own, pair, mid_i, mid_o, far_i, far_o, pre, near, far, far_cast):
    inner = is_inner()
    part = own.shape[0] // 2
    pre[...] = project((own[...], pair[...], either(inner, mid_i, mid_o), either(inner, far_i, far_o)), xs)
    gate = pre[:part, :]
    hidden = (gate * jax.nn.sigmoid(gate) * pre[part:, :]).astype(BF16)
    near[0] = dot(hidden, gs[0])
    near[1] = dot(hidden, gs[1])
    for p in range(2):
        block = dot(hidden, gs[2 + p])
        far[p] = block
        far_cast[p] = block.astype(BF16)


def pair_kernel(*refs):
    parts, ws, (out,), (cols,) = refs[:8], refs[8:12], refs[12:13], refs[13:]
    quarter, depth = parts[0].shape[0], cols.shape[2]

    @pl.when(is_inner())
    def _():
        for p, place in enumerate(line_places()):
            at = pl.ds(pl.multiple_of(place * depth, depth), depth)
            for i in range(8):
                cols[p, pl.ds(i * quarter, quarter), :] = parts[i][:, at]
        out[...] = project([w[...] for w in ws], cols).astype(BF16)


def back_kernel(gs, d0, d1, d2, d3, got, pre_a, pre_b, *refs):
    weights, (keep, give), (hid,) = (refs[:6], refs[6:12]), refs[12:14], refs[14:]
    inner = is_inner()
    half, count = hid.shape
    part, rows = half // 2, count // 4

    @pl.when(inner)
    def _():
        hid[...] = project((d0[...], d1[...], d2[...], d3[...]), gs)

    @pl.when(jnp.logical_not(inner))
    def _():
        hid[...] = got[...].astype(F32)

    grads = []
    for c, pre in enumerate((pre_a, pre_b)):
        _, gate_grad, up_grad = pointwise(pre[:part, :], pre[part:, :], hid[c * part:(c + 1) * part, :])
        grads.append(jnp.concatenate([gate_grad, up_grad], 0))
    width = keep.shape[-1]
    for p in range(4):
        total = None
        for c in range(2):
            own, pair, mid_i, mid_o, far_i, far_o = weights[c]
            w = (own[...], pair[...])[p] if p < 2 else either(inner, *((mid_i, mid_o), (far_i, far_o))[p - 2])
            term = contract_first(grads[c], w)
            total = term if total is None else total + term
        total = total.astype(BF16)
        at = pl.ds((p % 2) * (width // 2), width // 2)
        for group in range(2):
            base = group * 2 * rows
            keep[p // 2, group, :, at] = total[base:base + rows]
            give[p // 2, group, :, at] = total[base + rows:base + 2 * rows]


def place_kernel(*refs):
    parts, out = refs[:4], refs[4]
    quarters, places = token_quarters(), line_places()
    rows, width = parts[0].shape
    quarter, depth = rows // 2, width // 2
    for p in range(4):
        cols = pl.ds(pl.multiple_of(places[p] * depth, depth), depth)
        for i in range(4):
            at = pl.ds(pl.multiple_of(quarters[i] * quarter, quarter), quarter)
            source = parts[2 * (i // 2) + p // 2]
            out[at, cols] = source[(i % 2) * quarter:(i % 2 + 1) * quarter, (p % 2) * depth:(p % 2 + 1) * depth]


def paired_body(tokens, gate_weight, up_weight, down_weight, out_grad):
    y, t = lax.axis_index("rep"), lax.axis_index("tp")
    rows, width = tokens.shape
    units, depth = down_weight.shape
    half, quarter = units // 2, rows // 4
    part, count = half // 2, 2 * rows

    def my_part(w, c):
        return lax.dynamic_slice_in_dim(w, y * half + c * part, part, 0)

    gate_t, up_t = gate_weight.T, up_weight.T
    gu = [jnp.concatenate([my_part(gate_t, c), my_part(up_t, c)], 0) for c in range(2)]
    down_h = lax.dynamic_slice_in_dim(down_weight, y * half, half, 0)
    mine = [lax.dynamic_slice_in_dim(a, t * quarter, quarter, 0) for a in (tokens, out_grad)]

    p1a = lax.ppermute(gu[0], "fs", OUTER_PAIRS)
    p2a = lax.ppermute(gu[0], "fs", MIDDLE)
    p1b = lax.ppermute(gu[1], "fs", OUTER_PAIRS)
    p2b = lax.ppermute(gu[1], "fs", MIDDLE)
    q0 = lax.ppermute(jnp.stack(mine, 0), "rep", SWAP)
    p1d = lax.ppermute(down_h, "fs", INWARD)
    gp = [None] * 8
    gp[0] = lax.ppermute(mine[1], "fs", INWARD)
    p3a = lax.ppermute(p1a, "fs", MIDDLE)
    p4a = lax.ppermute(p2a, "fs", OUTWARD)
    p3b = lax.ppermute(p1b, "fs", MIDDLE)
    p4b = lax.ppermute(p2b, "fs", OUTWARD)
    q1 = lax.ppermute(q0, "tp", OVER_X)
    p2d = lax.ppermute(down_h, "fs", MIDDLE)
    q2 = lax.ppermute(q0, "tp", OVER_CORE)
    p5a = lax.ppermute(p3a, "fs", OUTWARD)
    p3d = lax.ppermute(p1d, "fs", MIDDLE)
    q3 = lax.ppermute(q1, "tp", OVER_CORE)
    gp[4] = lax.ppermute(gp[0], "rep", SWAP)
    p5b = lax.ppermute(p3b, "fs", OUTWARD)
    gp_x = lax.ppermute(jnp.stack([gp[0], gp[4]], 0), "tp", OVER_X)
    gp[1], gp[5] = gp_x[0], gp_x[1]
    for j in (0, 1, 4, 5):
        gp[j + 2] = lax.ppermute(gp[j], "tp", OVER_CORE)

    stacked = like((4, count, depth), BF16)
    xs, gs = call(lay_kernel, [stacked, stacked])(tokens, out_grad, q0, q1, q2, q3)
    gu_sets = ((gu[0], p1a, p2a, p4a, p3a, p5a), (gu[1], p1b, p2b, p4b, p3b, p5b))
    fronts = []
    for c in range(2):
        outs = [like((half, count), F32)] + [like((2, part, depth), d) for d in (F32, F32, BF16)]
        fronts.append(call(front_kernel, outs, flops=2 * count * width * (half + part))(xs, gs, *gu_sets[c]))
    gots = []
    for c in range(2):
        got = lax.ppermute(fronts[c][3], "fs", INWARD)
        gots.append((fronts[c][2] + got.astype(F32)).astype(BF16))

    down_pieces = (down_h, p1d, p2d, p3d)
    (pair_hid,) = call(
        pair_kernel, [like((half, count), BF16)], [pltpu.VMEM((4, count, depth), BF16)], flops=2 * count * width * half
    )(*gp, *down_pieces)
    hid_got = lax.ppermute(pair_hid, "fs", OUTWARD)

    gots = [lax.ppermute(gots[c], "fs", MIDDLE).astype(F32) for c in range(2)]
    keep, give = call(
        back_kernel,
        [like((2, 2, rows // 2, width // 2), BF16)] * 2,
        [pltpu.VMEM((half, count), F32)],
        flops=6 * count * width * half,
    )(gs, *down_pieces, hid_got, fronts[0][0], fronts[1][0], *gu_sets[0], *gu_sets[1])
    got = lax.ppermute(give, "tp", OVER_CORE)
    halved = (keep.astype(F32) + got.astype(F32)).astype(BF16)

    finals = []
    for c in range(2):
        near = fronts[c][1]
        last = lax.ppermute((near[1] + gots[c][1]).astype(BF16), "fs", OUTER_PAIRS).astype(F32)
        finals.append((near[0] + gots[c][0] + last).astype(BF16))
    peers = [lax.ppermute(finals[c], "rep", SWAP) for c in range(2)]
    final_own, peers = jnp.concatenate(finals, 0), jnp.concatenate(peers, 0)
    low = jnp.where(y == 0, final_own, peers)
    high = jnp.where(y == 0, peers, final_own)
    down_grad = jnp.concatenate([low, high], 0).astype(F32)
    wide = final_own.astype(F32)
    norm = jnp.sum(wide * wide, axis=1, keepdims=True).reshape(1, half)
    norm = norm + lax.ppermute(norm, "fs", OUTER_PAIRS)
    norm = norm + lax.ppermute(norm, "fs", ACROSS)
    norm_peer = lax.ppermute(norm, "rep", SWAP)
    norms = jnp.concatenate([jnp.where(y == 0, norm, norm_peer), jnp.where(y == 0, norm_peer, norm)], 1).reshape(units)

    done = []
    for i in range(2):
        got = lax.ppermute(halved[i, 1], "rep", SWAP)
        mine = (halved[i, 0].astype(F32) + got.astype(F32)).astype(BF16)
        got = lax.ppermute(mine, "tp", OVER_X)
        flipped = jnp.concatenate([got[quarter:], got[:quarter]], 0)
        done.append((mine.astype(F32) + flipped.astype(F32)).astype(BF16))
    done += [lax.ppermute(done[i], "tp", OVER_CORE) for i in range(2)]
    (input_grad,) = call(place_kernel, [like((rows, width), BF16)])(*done)
    return input_grad, down_grad, norms


def solution(mesh):
    sizes = dict(mesh.shape)
    line = (sizes["rep"], sizes["fs"], sizes["tp"]) == (2, 4, 4)
    return jax.shard_map(
        paired if line else gathered,
        mesh=mesh,
        in_specs=(
            P(("rep", "fs"), None),
            P("fs", "tp"),
            P("fs", "tp"),
            P("tp", "fs"),
            P(("rep", "fs"), None),
        ),
        out_specs=(P(("rep", "fs"), None), P("tp", "fs"), P("tp")),
        check_vma=False,
    )
```

```python
import functools

import jax
import jax.numpy as jnp
from jax import lax
from jax.experimental import pallas as pl
from jax.experimental.pallas import tpu as pltpu
from jax.sharding import PartitionSpec as P


F32, BF16 = jnp.float32, jnp.bfloat16


def contract_last(left, right):
    return lax.dot_general(left, right, (((1,), (1,)), ((), ())), preferred_element_type=F32)


def contract_first(left, right):
    return lax.dot_general(left, right, (((0,), (0,)), ((), ())), preferred_element_type=F32)


def gathered(tokens, gate_weight, up_weight, down_weight, out_grad):
    down_full = lax.all_gather(down_weight, "fs", axis=1, tiled=True)
    gate_full = lax.all_gather(gate_weight, "fs", axis=0, tiled=True)
    up_full = lax.all_gather(up_weight, "fs", axis=0, tiled=True)
    gate_pre = jnp.dot(tokens, gate_full, preferred_element_type=F32)
    up_pre = jnp.dot(tokens, up_full, preferred_element_type=F32)
    hid_grad = contract_last(out_grad, down_full)
    hidden, gate_grad, up_grad = pointwise(gate_pre, up_pre, hid_grad)
    partial_value = contract_last(gate_grad, gate_full) + contract_last(up_grad, up_full)
    input_grad = lax.psum(partial_value.astype(BF16), "tp")
    columns = lax.all_to_all(out_grad, "fs", split_axis=1, concat_axis=0, tiled=True)
    shard = contract_first(lax.all_gather(hidden, "fs", axis=0, tiled=True), columns)
    shard = lax.psum(shard.astype(BF16), "rep").astype(F32)
    norms = lax.psum(jnp.sum(shard * shard, axis=1), "fs")
    return input_grad, shard, norms


def pointwise(gate_pre, up_pre, hid_grad):
    sigma = jax.nn.sigmoid(gate_pre)
    activated = gate_pre * sigma
    hidden = (activated * up_pre).astype(BF16)
    up_grad = (hid_grad * activated).astype(BF16)
    gate_grad = (hid_grad * up_pre * sigma * (1.0 + gate_pre * (1.0 - sigma))).astype(BF16)
    return hidden, gate_grad, up_grad


OUTER_PAIRS = ((0, 1), (1, 0), (2, 3), (3, 2))
INWARD = ((0, 1), (3, 2))
OUTWARD = ((1, 0), (2, 3))
MIDDLE = ((1, 2), (2, 1))
ACROSS = ((0, 3), (3, 0), (1, 2), (2, 1))
SWAP = ((0, 1), (1, 0))
OVER_X = ((0, 2), (2, 0), (1, 3), (3, 1))
OVER_CORE = ((0, 1), (1, 0), (2, 3), (3, 2))

FIRST_CHUNK = 8


def paired(tokens, gate_weight, up_weight, down_weight, out_grad):
    return paired_body(tokens, gate_weight, up_weight, down_weight, out_grad)


def line_places():
    z = lax.axis_index("fs")
    return z, z + 1 - 2 * (z % 2), jnp.where(z < 2, 2, 1), jnp.where(z < 2, 3, 0)


def is_inner():
    z = lax.axis_index("fs")
    return jnp.logical_and(z > 0, z < 3)


def token_quarters():
    t = lax.axis_index("tp")
    x, c = t // 2, t % 2
    return t, 2 * (1 - x) + c, 2 * x + 1 - c, 3 - t


def call(kernel, outs, scratch=(), flops=0, limit=28):
    def inner_call(*args):
        size = sum(v.size * v.dtype.itemsize for v in args)
        return pl.pallas_call(
            kernel,
            out_shape=outs,
            in_specs=[pl.BlockSpec(memory_space=pltpu.VMEM)] * len(args),
            out_specs=[pl.BlockSpec(memory_space=pltpu.VMEM)] * len(outs),
            scratch_shapes=list(scratch),
            compiler_params=pltpu.CompilerParams(vmem_limit_bytes=limit * 2**20),
            cost_estimate=pl.CostEstimate(flops=flops, bytes_accessed=size, transcendentals=0),
        )(*args)

    return inner_call


def like(shape, dtype):
    return jax.ShapeDtypeStruct(shape, dtype)


def lay_kernel(tok, grad, *refs):
    others, (xs, gs) = refs[:4], refs[4:]
    depth, quarter = xs.shape[2], others[0].shape[1]
    quarters = token_quarters()
    for p, place in enumerate(line_places()):
        cols = pl.ds(pl.multiple_of(place * depth, depth), depth)
        for i in range(4):
            rows = pl.ds(pl.multiple_of(quarters[i] * quarter, quarter), quarter)
            here, there = pl.ds(i * quarter, quarter), pl.ds((4 + i) * quarter, quarter)
            xs[p, here, :] = tok[rows, cols]
            gs[p, here, :] = grad[rows, cols]
            xs[p, there, :] = others[i][0, :, cols]
            gs[p, there, :] = others[i][1, :, cols]


def either(inner, a, b):
    return jnp.where(inner, a[...], b[...])


def dot(a, b):
    return jnp.dot(a, b, preferred_element_type=F32)


def project(ws, cols):
    return sum(contract_last(w, cols[p]) for p, w in enumerate(ws))


def front_kernel(xs, gs, own, pair, mid_i, mid_o, far_i, far_o, pre, near, far, far_cast):
    inner = is_inner()
    part = own.shape[0] // 2
    pre[...] = project((own[...], pair[...], either(inner, mid_i, mid_o), either(inner, far_i, far_o)), xs)
    gate = pre[:part, :]
    hidden = (gate * jax.nn.sigmoid(gate) * pre[part:, :]).astype(BF16)
    near[0] = dot(hidden, gs[0])
    near[1] = dot(hidden, gs[1])
    for p in range(2):
        block = dot(hidden, gs[2 + p])
        far[p] = block
        far_cast[p] = block.astype(BF16)


def pair_kernel(*refs):
    groups, ws, (out,), (cols,) = refs[:4], refs[4:8], refs[8:9], refs[9:]
    quarter, depth = groups[0].shape[0], cols.shape[2]

    @pl.when(is_inner())
    def _():
        for p, place in enumerate(line_places()):
            at = pl.ds(pl.multiple_of(place * depth, depth), depth)
            for i in range(4):
                cols[p, pl.ds(i * quarter, quarter), :] = groups[i][:, at]
        out[...] = project([w[...] for w in ws], cols).astype(BF16)


def own_kernel(gs, d0, d1, d2, d3, out):
    @pl.when(is_inner())
    def _():
        out[...] = project((d0[...], d1[...], d2[...], d3[...]), gs)


def back_kernel(group, parts, hid_own, got, pre_a, pre_b, *refs):
    weights, (keep, give), (hid,) = (refs[:6], refs[6:12]), refs[12:14], refs[14:]
    inner = is_inner()
    count = hid.shape[1]
    tok = slice(group * count, (group + 1) * count)

    @pl.when(inner)
    def _():
        hid[...] = hid_own[:, tok]

    @pl.when(jnp.logical_not(inner))
    def _():
        hid[...] = got[...].astype(F32)

    grads = []
    begin = 0
    for part, pre in zip(parts, (pre_a, pre_b)):
        _, gate_grad, up_grad = pointwise(pre[:part, tok], pre[part:, tok], hid[begin:begin + part, :])
        begin += part
        grads.append(jnp.concatenate([gate_grad, up_grad], 0))
    rows, depth = keep.shape[1], keep.shape[2] // 2
    for p in range(4):
        total = None
        for c in range(2):
            own, pair, mid_i, mid_o, far_i, far_o = weights[c]
            w = (own[...], pair[...])[p] if p < 2 else either(inner, *((mid_i, mid_o), (far_i, far_o))[p - 2])
            term = contract_first(grads[c], w)
            total = term if total is None else total + term
        total = total.astype(BF16)
        at = pl.ds((p % 2) * depth, depth)
        keep[p // 2, :, at] = total[:rows]
        give[p // 2, :, at] = total[rows:]


def near_kernel(near, got, owned, paired_sum):
    owned[...] = near[0] + got[0].astype(F32)
    paired_sum[...] = (near[1] + got[1].astype(F32)).astype(BF16)


def add_kernel(a, b, out):
    out[...] = (a[...].astype(F32) + b[...].astype(F32)).astype(out.dtype)


def add_halves_kernel(a, b, *outs):
    for i, out in enumerate(outs):
        out[...] = (a[i].astype(F32) + b[i].astype(F32)).astype(BF16)


def add_flipped_kernel(a, b, out):
    half = a.shape[0] // 2
    out[:half] = (a[:half].astype(F32) + b[half:].astype(F32)).astype(BF16)
    out[half:] = (a[half:].astype(F32) + b[:half].astype(F32)).astype(BF16)


def place_kernel(*refs):
    parts, out = refs[:4], refs[4]
    quarters, places = token_quarters(), line_places()
    rows, width = parts[0].shape
    quarter, depth = rows // 2, width // 2
    for p in range(4):
        cols = pl.ds(pl.multiple_of(places[p] * depth, depth), depth)
        for i in range(4):
            at = pl.ds(pl.multiple_of(quarters[i] * quarter, quarter), quarter)
            source = parts[2 * (i // 2) + p // 2]
            out[at, cols] = source[(i % 2) * quarter:(i % 2 + 1) * quarter, (p % 2) * depth:(p % 2 + 1) * depth]


def paired_body(tokens, gate_weight, up_weight, down_weight, out_grad):
    y, t = lax.axis_index("rep"), lax.axis_index("tp")
    rows, width = tokens.shape
    units, depth = down_weight.shape
    half, quarter = units // 2, rows // 4
    count = 2 * rows
    long = half * FIRST_CHUNK // 16 // 16 * 16
    parts, begins = (long, half - long), (0, long)

    def my_part(w, c):
        return lax.dynamic_slice_in_dim(w, y * half + begins[c], parts[c], 0)

    gate_t, up_t = gate_weight.T, up_weight.T
    gu = [jnp.concatenate([my_part(gate_t, c), my_part(up_t, c)], 0) for c in range(2)]
    down_h = lax.dynamic_slice_in_dim(down_weight, y * half, half, 0)
    mine = [lax.dynamic_slice_in_dim(a, t * quarter, quarter, 0) for a in (tokens, out_grad)]

    p1a = lax.ppermute(gu[0], "fs", OUTER_PAIRS)
    p2a = lax.ppermute(gu[0], "fs", MIDDLE)
    p1b = lax.ppermute(gu[1], "fs", OUTER_PAIRS)
    p2b = lax.ppermute(gu[1], "fs", MIDDLE)
    q0 = lax.ppermute(jnp.stack(mine, 0), "rep", SWAP)
    p1d = lax.ppermute(down_h, "fs", INWARD)
    gp = [None] * 8
    gp[0] = lax.ppermute(mine[1], "fs", INWARD)
    p3a = lax.ppermute(p1a, "fs", MIDDLE)
    p4a = lax.ppermute(p2a, "fs", OUTWARD)
    p3b = lax.ppermute(p1b, "fs", MIDDLE)
    p4b = lax.ppermute(p2b, "fs", OUTWARD)
    q1 = lax.ppermute(q0, "tp", OVER_X)
    p2d = lax.ppermute(down_h, "fs", MIDDLE)
    q2 = lax.ppermute(q0, "tp", OVER_CORE)
    p5a = lax.ppermute(p3a, "fs", OUTWARD)
    p3d = lax.ppermute(p1d, "fs", MIDDLE)
    q3 = lax.ppermute(q1, "tp", OVER_CORE)
    gp[4] = lax.ppermute(gp[0], "rep", SWAP)
    p5b = lax.ppermute(p3b, "fs", OUTWARD)
    gp_x = lax.ppermute(jnp.stack([gp[0], gp[4]], 0), "tp", OVER_X)
    gp[1], gp[5] = gp_x[0], gp_x[1]
    for j in (0, 1, 4, 5):
        gp[j + 2] = lax.ppermute(gp[j], "tp", OVER_CORE)

    stacked = like((4, count, depth), BF16)
    xs, gs = call(lay_kernel, [stacked, stacked])(tokens, out_grad, q0, q1, q2, q3)
    gu_sets = ((gu[0], p1a, p2a, p4a, p3a, p5a), (gu[1], p1b, p2b, p4b, p3b, p5b))
    fronts = []
    for c in range(2):
        outs = [like((2 * parts[c], count), F32)] + [like((2, parts[c], depth), d) for d in (F32, F32, BF16)]
        fronts.append(call(front_kernel, outs, flops=6 * count * width * parts[c])(xs, gs, *gu_sets[c]))
    gots = []
    for c in range(2):
        got = lax.ppermute(fronts[c][3], "fs", INWARD)
        far = fronts[c][2]
        gots += call(add_kernel, [like(far.shape, BF16)])(far, got)

    down_pieces = (down_h, p1d, p2d, p3d)
    hid_gots = [None, None]
    for group in (1, 0):
        (pair_hid,) = call(
            pair_kernel, [like((half, rows), BF16)], [pltpu.VMEM((4, rows, depth), BF16)], flops=2 * rows * width * half
        )(*gp[4 * group:4 * group + 4], *down_pieces)
        hid_gots[group] = lax.ppermute(pair_hid, "fs", OUTWARD)
    (own_hid,) = call(own_kernel, [like((half, count), F32)], flops=2 * count * width * half)(gs, *down_pieces)

    gots = [lax.ppermute(gots[c], "fs", MIDDLE) for c in range(2)]
    halves = [None, None]
    for group in (1, 0):
        keep, give = call(
            functools.partial(back_kernel, group, parts),
            [like((2, rows // 2, width // 2), BF16)] * 2,
            [pltpu.VMEM((half, rows), F32)],
            flops=4 * rows * width * half,
        )(own_hid, hid_gots[group], fronts[0][0], fronts[1][0], *gu_sets[0], *gu_sets[1])
        got = lax.ppermute(give, "tp", OVER_CORE)
        halves[group] = call(add_halves_kernel, [like(keep.shape[1:], BF16)] * 2)(keep, got)

    finals = []
    for c in range(2):
        block = gots[c].shape[1:]
        owned, paired_sum = call(near_kernel, [like(block, F32), like(block, BF16)])(fronts[c][1], gots[c])
        last = lax.ppermute(paired_sum, "fs", OUTER_PAIRS)
        finals += call(add_kernel, [like(block, BF16)])(owned, last)
    peers = [lax.ppermute(finals[c], "rep", SWAP) for c in range(2)]
    final_own, peers = jnp.concatenate(finals, 0), jnp.concatenate(peers, 0)
    low = jnp.where(y == 0, final_own, peers)
    high = jnp.where(y == 0, peers, final_own)
    down_grad = jnp.concatenate([low, high], 0).astype(F32)
    wide = final_own.astype(F32)
    norm = jnp.sum(wide * wide, axis=1, keepdims=True).reshape(1, half)
    norm = norm + lax.ppermute(norm, "fs", OUTER_PAIRS)
    norm = norm + lax.ppermute(norm, "fs", ACROSS)
    norm_peer = lax.ppermute(norm, "rep", SWAP)
    norms = jnp.concatenate([jnp.where(y == 0, norm, norm_peer), jnp.where(y == 0, norm_peer, norm)], 1).reshape(units)

    done = []
    for i in range(2):
        got = lax.ppermute(halves[1][i], "rep", SWAP)
        (mine,) = call(add_kernel, [like(got.shape, BF16)])(halves[0][i], got)
        got = lax.ppermute(mine, "tp", OVER_X)
        done += call(add_flipped_kernel, [like(got.shape, BF16)])(mine, got)
    done += [lax.ppermute(done[i], "tp", OVER_CORE) for i in range(2)]
    (input_grad,) = call(place_kernel, [like((rows, width), BF16)])(*done)
    return input_grad, down_grad, norms


def solution(mesh):
    sizes = dict(mesh.shape)
    line = (sizes["rep"], sizes["fs"], sizes["tp"]) == (2, 4, 4)
    return jax.shard_map(
        paired if line else gathered,
        mesh=mesh,
        in_specs=(
            P(("rep", "fs"), None),
            P("fs", "tp"),
            P("fs", "tp"),
            P("tp", "fs"),
            P(("rep", "fs"), None),
        ),
        out_specs=(P(("rep", "fs"), None), P("tp", "fs"), P("tp")),
        check_vma=False,
    )
```

```python
import functools

import jax
import jax.numpy as jnp
from jax import lax
from jax.experimental import pallas as pl
from jax.experimental.pallas import tpu as pltpu
from jax.sharding import PartitionSpec as P


F32, BF16 = jnp.float32, jnp.bfloat16


def contract_last(left, right):
    return lax.dot_general(left, right, (((1,), (1,)), ((), ())), preferred_element_type=F32)


def contract_first(left, right):
    return lax.dot_general(left, right, (((0,), (0,)), ((), ())), preferred_element_type=F32)


def gathered(tokens, gate_weight, up_weight, down_weight, out_grad):
    down_full = lax.all_gather(down_weight, "fs", axis=1, tiled=True)
    gate_full = lax.all_gather(gate_weight, "fs", axis=0, tiled=True)
    up_full = lax.all_gather(up_weight, "fs", axis=0, tiled=True)
    gate_pre = jnp.dot(tokens, gate_full, preferred_element_type=F32)
    up_pre = jnp.dot(tokens, up_full, preferred_element_type=F32)
    hid_grad = contract_last(out_grad, down_full)
    hidden, gate_grad, up_grad = pointwise(gate_pre, up_pre, hid_grad)
    partial_value = contract_last(gate_grad, gate_full) + contract_last(up_grad, up_full)
    input_grad = lax.psum(partial_value.astype(BF16), "tp")
    columns = lax.all_to_all(out_grad, "fs", split_axis=1, concat_axis=0, tiled=True)
    shard = contract_first(lax.all_gather(hidden, "fs", axis=0, tiled=True), columns)
    shard = lax.psum(shard.astype(BF16), "rep").astype(F32)
    norms = lax.psum(jnp.sum(shard * shard, axis=1), "fs")
    return input_grad, shard, norms


def pointwise(gate_pre, up_pre, hid_grad):
    sigma = jax.nn.sigmoid(gate_pre)
    activated = gate_pre * sigma
    hidden = (activated * up_pre).astype(BF16)
    up_grad = (hid_grad * activated).astype(BF16)
    gate_grad = (hid_grad * up_pre * sigma * (1.0 + gate_pre * (1.0 - sigma))).astype(BF16)
    return hidden, gate_grad, up_grad


OUTER_PAIRS = ((0, 1), (1, 0), (2, 3), (3, 2))
INWARD = ((0, 1), (3, 2))
OUTWARD = ((1, 0), (2, 3))
MIDDLE = ((1, 2), (2, 1))
ACROSS = ((0, 3), (3, 0), (1, 2), (2, 1))
SWAP = ((0, 1), (1, 0))
OVER_X = ((0, 2), (2, 0), (1, 3), (3, 1))
OVER_CORE = ((0, 1), (1, 0), (2, 3), (3, 2))

FIRST_CHUNK = 8


def paired(tokens, gate_weight, up_weight, down_weight, out_grad):
    return paired_body(tokens, gate_weight, up_weight, down_weight, out_grad)


def line_places():
    z = lax.axis_index("fs")
    return z, z + 1 - 2 * (z % 2), jnp.where(z < 2, 2, 1), jnp.where(z < 2, 3, 0)


def is_inner():
    z = lax.axis_index("fs")
    return jnp.logical_and(z > 0, z < 3)


def token_quarters():
    t = lax.axis_index("tp")
    x, c = t // 2, t % 2
    return t, 2 * (1 - x) + c, 2 * x + 1 - c, 3 - t


def call(kernel, outs, scratch=(), flops=0, limit=28):
    def inner_call(*args):
        size = sum(v.size * v.dtype.itemsize for v in args)
        return pl.pallas_call(
            kernel,
            out_shape=outs,
            in_specs=[pl.BlockSpec(memory_space=pltpu.VMEM)] * len(args),
            out_specs=[pl.BlockSpec(memory_space=pltpu.VMEM)] * len(outs),
            scratch_shapes=list(scratch),
            compiler_params=pltpu.CompilerParams(vmem_limit_bytes=limit * 2**20),
            cost_estimate=pl.CostEstimate(flops=flops, bytes_accessed=size, transcendentals=0),
        )(*args)

    return inner_call


def like(shape, dtype):
    return jax.ShapeDtypeStruct(shape, dtype)


def lay_kernel(tok, grad, *refs):
    others, (xs, gs) = refs[:4], refs[4:]
    depth, quarter = xs.shape[2], others[0].shape[1]
    quarters = token_quarters()
    for p, place in enumerate(line_places()):
        cols = pl.ds(pl.multiple_of(place * depth, depth), depth)
        for i in range(4):
            rows = pl.ds(pl.multiple_of(quarters[i] * quarter, quarter), quarter)
            here, there = pl.ds(i * quarter, quarter), pl.ds((4 + i) * quarter, quarter)
            xs[p, here, :] = tok[rows, cols]
            gs[p, here, :] = grad[rows, cols]
            xs[p, there, :] = others[i][0, :, cols]
            gs[p, there, :] = others[i][1, :, cols]


def either(inner, a, b):
    return jnp.where(inner, a[...], b[...])


def dot(a, b):
    return jnp.dot(a, b, preferred_element_type=F32)


def project(ws, cols):
    return sum(contract_last(w, cols[p]) for p, w in enumerate(ws))


def front_kernel(xs, gs, own, pair, mid_i, mid_o, far_i, far_o, pre, near, far, far_cast):
    inner = is_inner()
    part = own.shape[0] // 2
    pre[...] = project((own[...], pair[...], either(inner, mid_i, mid_o), either(inner, far_i, far_o)), xs)
    gate = pre[:part, :]
    hidden = (gate * jax.nn.sigmoid(gate) * pre[part:, :]).astype(BF16)
    for p in range(2):
        block = dot(hidden, gs[2 + p])
        far[p] = block
        far_cast[p] = block.astype(BF16)
    near[0] = dot(hidden, gs[0])
    near[1] = dot(hidden, gs[1])


def pair_kernel(*refs):
    groups, ws, (out,), (cols,) = refs[:4], refs[4:8], refs[8:9], refs[9:]
    quarter, depth = groups[0].shape[0], cols.shape[2]

    @pl.when(is_inner())
    def _():
        for p, place in enumerate(line_places()):
            at = pl.ds(pl.multiple_of(place * depth, depth), depth)
            for i in range(4):
                cols[p, pl.ds(i * quarter, quarter), :] = groups[i][:, at]
        out[...] = project([w[...] for w in ws], cols).astype(BF16)


def own_kernel(gs, d0, d1, d2, d3, out):
    @pl.when(is_inner())
    def _():
        out[...] = project((d0[...], d1[...], d2[...], d3[...]), gs)


def back_kernel(group, parts, hid_own, got, pre_a, pre_b, *refs):
    weights, (keep, give), (hid,) = (refs[:6], refs[6:12]), refs[12:14], refs[14:]
    inner = is_inner()
    count = hid.shape[1]
    tok = slice(group * count, (group + 1) * count)

    @pl.when(inner)
    def _():
        hid[...] = hid_own[:, tok]

    @pl.when(jnp.logical_not(inner))
    def _():
        hid[...] = got[...].astype(F32)

    grads = []
    begin = 0
    for part, pre in zip(parts, (pre_a, pre_b)):
        _, gate_grad, up_grad = pointwise(pre[:part, tok], pre[part:, tok], hid[begin:begin + part, :])
        begin += part
        grads.append(jnp.concatenate([gate_grad, up_grad], 0))
    rows, depth = keep.shape[1], keep.shape[2] // 2
    for p in range(4):
        total = None
        for c in range(2):
            own, pair, mid_i, mid_o, far_i, far_o = weights[c]
            w = (own[...], pair[...])[p] if p < 2 else either(inner, *((mid_i, mid_o), (far_i, far_o))[p - 2])
            term = contract_first(grads[c], w)
            total = term if total is None else total + term
        total = total.astype(BF16)
        at = pl.ds((p % 2) * depth, depth)
        keep[p // 2, :, at] = total[:rows]
        give[p // 2, :, at] = total[rows:]


def near_kernel(near, got, owned, paired_sum):
    owned[...] = near[0] + got[0].astype(F32)
    paired_sum[...] = (near[1] + got[1].astype(F32)).astype(BF16)


def pair_add_kernel(near, got, out):
    out[...] = (near[1] + got[...].astype(F32)).astype(BF16)


def own_add_kernel(near, got, last, out):
    out[...] = (near[0] + got[...].astype(F32) + last[...].astype(F32)).astype(BF16)


def add_kernel(a, b, out):
    out[...] = (a[...].astype(F32) + b[...].astype(F32)).astype(out.dtype)


def add_halves_kernel(a, b, *outs):
    for i, out in enumerate(outs):
        out[...] = (a[i].astype(F32) + b[i].astype(F32)).astype(BF16)


def add_flipped_kernel(a, b, out):
    half = a.shape[0] // 2
    out[:half] = (a[:half].astype(F32) + b[half:].astype(F32)).astype(BF16)
    out[half:] = (a[half:].astype(F32) + b[:half].astype(F32)).astype(BF16)


def place_kernel(*refs):
    parts, out = refs[:4], refs[4]
    quarters, places = token_quarters(), line_places()
    rows, width = parts[0].shape
    quarter, depth = rows // 2, width // 2
    for p in range(4):
        cols = pl.ds(pl.multiple_of(places[p] * depth, depth), depth)
        for i in range(4):
            at = pl.ds(pl.multiple_of(quarters[i] * quarter, quarter), quarter)
            source = parts[2 * (i // 2) + p // 2]
            out[at, cols] = source[(i % 2) * quarter:(i % 2 + 1) * quarter, (p % 2) * depth:(p % 2 + 1) * depth]


def paired_body(tokens, gate_weight, up_weight, down_weight, out_grad):
    y, t = lax.axis_index("rep"), lax.axis_index("tp")
    rows, width = tokens.shape
    units, depth = down_weight.shape
    half, quarter = units // 2, rows // 4
    count = 2 * rows
    long = half * FIRST_CHUNK // 16 // 16 * 16
    parts, begins = (long, half - long), (0, long)

    def my_part(w, c):
        return lax.dynamic_slice_in_dim(w, y * half + begins[c], parts[c], 0)

    gate_t, up_t = gate_weight.T, up_weight.T
    gu = [jnp.concatenate([my_part(gate_t, c), my_part(up_t, c)], 0) for c in range(2)]
    down_h = lax.dynamic_slice_in_dim(down_weight, y * half, half, 0)
    mine = [lax.dynamic_slice_in_dim(a, t * quarter, quarter, 0) for a in (tokens, out_grad)]

    p1a = lax.ppermute(gu[0], "fs", OUTER_PAIRS)
    p2a = lax.ppermute(gu[0], "fs", MIDDLE)
    p1b = lax.ppermute(gu[1], "fs", OUTER_PAIRS)
    p2b = lax.ppermute(gu[1], "fs", MIDDLE)
    q0 = lax.ppermute(jnp.stack(mine, 0), "rep", SWAP)
    p1d = lax.ppermute(down_h, "fs", INWARD)
    gp = [None] * 8
    gp[0] = lax.ppermute(mine[1], "fs", INWARD)
    p3a = lax.ppermute(p1a, "fs", MIDDLE)
    p4a = lax.ppermute(p2a, "fs", OUTWARD)
    p3b = lax.ppermute(p1b, "fs", MIDDLE)
    p4b = lax.ppermute(p2b, "fs", OUTWARD)
    q1 = lax.ppermute(q0, "tp", OVER_X)
    p2d = lax.ppermute(down_h, "fs", MIDDLE)
    q2 = lax.ppermute(q0, "tp", OVER_CORE)
    p5a = lax.ppermute(p3a, "fs", OUTWARD)
    p3d = lax.ppermute(p1d, "fs", MIDDLE)
    q3 = lax.ppermute(q1, "tp", OVER_CORE)
    gp[4] = lax.ppermute(gp[0], "rep", SWAP)
    p5b = lax.ppermute(p3b, "fs", OUTWARD)
    gp_x = lax.ppermute(jnp.stack([gp[0], gp[4]], 0), "tp", OVER_X)
    gp[1], gp[5] = gp_x[0], gp_x[1]
    for j in (0, 1, 4, 5):
        gp[j + 2] = lax.ppermute(gp[j], "tp", OVER_CORE)

    stacked = like((4, count, depth), BF16)
    xs, gs = call(lay_kernel, [stacked, stacked])(tokens, out_grad, q0, q1, q2, q3)
    gu_sets = ((gu[0], p1a, p2a, p4a, p3a, p5a), (gu[1], p1b, p2b, p4b, p3b, p5b))
    fronts = []
    for c in range(2):
        outs = [like((2 * parts[c], count), F32)] + [like((2, parts[c], depth), d) for d in (F32, F32, BF16)]
        fronts.append(call(front_kernel, outs, flops=6 * count * width * parts[c])(xs, gs, *gu_sets[c]))
    far, cast = fronts[0][2:]
    got = lax.ppermute(cast, "fs", INWARD)
    (far,) = call(add_kernel, [like(far.shape, BF16)])(far, got)
    from_a = lax.ppermute(far, "fs", MIDDLE)
    far, cast = fronts[1][2:]
    got = lax.ppermute(cast, "fs", INWARD)
    far_in, far_out = call(add_halves_kernel, [like(far.shape[1:], BF16)] * 2)(far, got)
    from_bc = lax.ppermute(far_out, "fs", MIDDLE)
    from_bb = lax.ppermute(far_in, "fs", MIDDLE)

    down_pieces = (down_h, p1d, p2d, p3d)
    hid_gots = [None, None]
    for group in (1, 0):
        (pair_hid,) = call(
            pair_kernel, [like((half, rows), BF16)], [pltpu.VMEM((4, rows, depth), BF16)], flops=2 * rows * width * half
        )(*gp[4 * group:4 * group + 4], *down_pieces)
        hid_gots[group] = lax.ppermute(pair_hid, "fs", OUTWARD)
    (own_hid,) = call(own_kernel, [like((half, count), F32)], flops=2 * count * width * half)(gs, *down_pieces)

    halves = [None, None]
    for group in (1, 0):
        keep, give = call(
            functools.partial(back_kernel, group, parts),
            [like((2, rows // 2, width // 2), BF16)] * 2,
            [pltpu.VMEM((half, rows), F32)],
            flops=4 * rows * width * half,
        )(own_hid, hid_gots[group], fronts[0][0], fronts[1][0], *gu_sets[0], *gu_sets[1])
        got = lax.ppermute(give, "tp", OVER_CORE)
        halves[group] = call(add_halves_kernel, [like(keep.shape[1:], BF16)] * 2)(keep, got)

    near_a, near_b = fronts[0][1], fronts[1][1]
    owned, paired_a = call(near_kernel, [like(near_a.shape[1:], d) for d in (F32, BF16)])(near_a, from_a)
    (paired_b,) = call(pair_add_kernel, [like(near_b.shape[1:], BF16)])(near_b, from_bc)
    last_a = lax.ppermute(paired_a, "fs", OUTER_PAIRS)
    last_b = lax.ppermute(paired_b, "fs", OUTER_PAIRS)
    finals = call(add_kernel, [like(owned.shape, BF16)])(owned, last_a)
    finals += call(own_add_kernel, [like(paired_b.shape, BF16)])(near_b, from_bb, last_b)
    peers = [lax.ppermute(finals[c], "rep", SWAP) for c in range(2)]
    final_own, peers = jnp.concatenate(finals, 0), jnp.concatenate(peers, 0)
    low = jnp.where(y == 0, final_own, peers)
    high = jnp.where(y == 0, peers, final_own)
    down_grad = jnp.concatenate([low, high], 0).astype(F32)
    wide = final_own.astype(F32)
    norm = jnp.sum(wide * wide, axis=1, keepdims=True).reshape(1, half)
    norm = norm + lax.ppermute(norm, "fs", OUTER_PAIRS)
    norm = norm + lax.ppermute(norm, "fs", ACROSS)
    norm_peer = lax.ppermute(norm, "rep", SWAP)
    norms = jnp.concatenate([jnp.where(y == 0, norm, norm_peer), jnp.where(y == 0, norm_peer, norm)], 1).reshape(units)

    done = []
    for i in range(2):
        got = lax.ppermute(halves[1][i], "rep", SWAP)
        (mine,) = call(add_kernel, [like(got.shape, BF16)])(halves[0][i], got)
        got = lax.ppermute(mine, "tp", OVER_X)
        done += call(add_flipped_kernel, [like(got.shape, BF16)])(mine, got)
    done += [lax.ppermute(done[i], "tp", OVER_CORE) for i in range(2)]
    (input_grad,) = call(place_kernel, [like((rows, width), BF16)])(*done)
    return input_grad, down_grad, norms


def solution(mesh):
    sizes = dict(mesh.shape)
    line = (sizes["rep"], sizes["fs"], sizes["tp"]) == (2, 4, 4)
    return jax.shard_map(
        paired if line else gathered,
        mesh=mesh,
        in_specs=(
            P(("rep", "fs"), None),
            P("fs", "tp"),
            P("fs", "tp"),
            P("tp", "fs"),
            P(("rep", "fs"), None),
        ),
        out_specs=(P(("rep", "fs"), None), P("tp", "fs"), P("tp")),
        check_vma=False,
    )
```
